256 devices in a mesh: ep: 16 (over y, x), tp: 16 (over z, core).
Axes of the slice: x: 4, y: 4, z: 8, core: 2. Of those that a mesh axis runs over, the one named last changes fastest.
Arguments:
- tokens: bfloat16 [8192, 1024], P(('ep', 'tp')), may hold values from -6 to 6
- norm_gain: float32 [1024], replicated, may hold values from 0.5 to 1.5
- routing: int32 [8192, 2], P('ep'), may hold values from 0 to 31, as said below
- gate_share: float32 [8192, 2], P('ep'), may hold values from 0.5 to 1.5
- w_gate: bfloat16 [32, 1024, 256], P('ep', None, 'tp'), may hold values from -0.1875 to 0.1875
- w_up: bfloat16 [32, 1024, 256], P('ep', None, 'tp'), may hold values from -0.1875 to 0.1875
- w_down: bfloat16 [32, 256, 1024], P('ep', 'tp'), may hold values from -0.375 to 0.375
Outputs:
- mixed_out: bfloat16 [8192, 1024], P('ep', 'tp')
The draws below stay inside these ranges and needn't reach their ends.
Inputs may be any that keep to these rules, and one draw needn't show every extreme that they name: `routing`: each row names two different experts whose ids lie in the same block of 8 consecutive ids. In each aligned block of 512 rows (the tokens of one index of ep) no expert is named by more than 64 rows, and some expert is named by exactly 64.
All inputs are finite; a program needn't handle non-finite values.
Results may differ from the reference program's by a relative error of at most 0.0015.
Values may be sent and summed in bfloat16 or wider, within the bound.
No kernel may reach another device: no remote copies, remote signals or barrier semaphores. Data moves between devices by JAX's collectives and lax.ppermute only.
A program may use at most 64 MiB of HBM per device.

```python
import jax
import jax.numpy as jnp
from jax import lax

D = 1024
HIDDEN_SIZE = 256
TOPK = 2
GROUPS = 4
GROUP_TOK = 512
TOKENS = 8192
EXPERTS = 32
CAP = 64
N_EP = 16


def draw_routing(key, part):
    block_count = TOKENS // GROUP_TOK
    group_size = EXPERTS // GROUPS
    eighth = GROUP_TOK // 8
    position = jnp.arange(GROUP_TOK, dtype=jnp.int32)
    group_slot = (position >= 4 * eighth).astype(jnp.int32) + (position >= 6 * eighth).astype(jnp.int32) + (position >= 7 * eighth).astype(jnp.int32)
    group_start = jnp.array([0, 4 * eighth, 6 * eighth, 7 * eighth], dtype=jnp.int32)[group_slot]
    within = position - group_start
    first_pick = within % group_size
    second = (within + 1) % group_size

    def inner_draw(sub_key):
        return jax.random.permutation(sub_key, group_size).astype(jnp.int32)

    def draw_block(block_key):
        key_order, key_group, key_inner, key_flip = jax.random.split(block_key, 4)
        token_order = jax.random.permutation(key_order, GROUP_TOK).astype(jnp.int32)
        group_label = jax.random.permutation(key_group, GROUPS).astype(jnp.int32)
        inner_order = jax.vmap(inner_draw)(jax.random.split(key_inner, GROUPS))
        label = group_label[group_slot]
        one_id = label * group_size + inner_order[label, first_pick]
        two_id = label * group_size + inner_order[label, second]
        flipped = jax.random.randint(key_flip, (GROUP_TOK,), 0, 2)
        left = jnp.where(flipped == 1, two_id, one_id)
        right = jnp.where(flipped == 1, one_id, two_id)
        paired = jnp.stack([left, right], axis=1)
        return paired[token_order].astype(jnp.int32)
    block_keys = jax.random.split(jax.random.fold_in(key, 11), block_count)
    return jax.vmap(draw_block)(block_keys).reshape(TOKENS, 2).astype(jnp.int32)


def level_of(stream_key, shape, shards, low, high):
    def one(dim, parts):
        draws = jax.random.uniform(jax.random.fold_in(jax.random.fold_in(stream_key, 6), dim), (parts,), jnp.float32, low / len(shards), high / len(shards))
        return jnp.repeat(jnp.exp(draws), shape[dim] // parts).reshape((-1,) + (1,) * (len(shape) - dim - 1))

    gain = one(*shards[0])
    for cut in shards[1:]:
        gain = gain * one(*cut)
    return gain


def gaussian(stream_key, dims, spread, bound, pieces=(), kind=jnp.bfloat16):
    entries = jax.random.normal(stream_key, dims, jnp.float32) * spread
    if len(pieces) > 0:
        entries = level_of(stream_key, dims, pieces, -0.22, 0.18) * entries
    return jnp.clip(entries, min=-bound, max=bound).astype(kind)


def setup_inputs(seed: int = 0) -> dict:
    seeds = jax.random.split(jax.random.key(seed), 8)
    tokens = gaussian(seeds[0], (TOKENS, D), 1.0, 6.0, ((0, 256),))
    norm_gain = jnp.clip(1.0 + 0.1 * jax.random.normal(seeds[1], (D,), jnp.float32), 0.5, 1.5)
    routing = draw_routing(jax.random.fold_in(seeds[7], 71), 0)
    gate_share = jnp.clip(0.5 + 1.0 * jax.random.uniform(seeds[3], (TOKENS, TOPK), jnp.float32) ** level_of(seeds[3], (TOKENS, TOPK), ((0, 16),), -0.2, 0.2), 0.5, 1.5)
    w_gate = gaussian(seeds[4], (EXPERTS, D, HIDDEN_SIZE), D ** -0.5, 0.1875, ((0, 16), (2, 16)))
    w_up = gaussian(seeds[5], (EXPERTS, D, HIDDEN_SIZE), D ** -0.5, 0.1875, ((0, 16), (2, 16)))
    w_down = gaussian(seeds[6], (EXPERTS, HIDDEN_SIZE, D), HIDDEN_SIZE ** -0.5, 0.375, ((0, 16), (1, 16)))
    return {"tokens": tokens, "norm_gain": norm_gain, "routing": routing, "gate_share": gate_share, "w_gate": w_gate, "w_up": w_up, "w_down": w_down}


epsilon = 1e-06

def norm_rows(tokens, norm_gain):
    as_float = tokens.astype(jnp.float32)
    scaled = as_float * lax.rsqrt(lax.optimization_barrier(jnp.mean(as_float * as_float, axis=-1, keepdims=True)) + epsilon)
    return (scaled * norm_gain.astype(jnp.float32)).astype(jnp.bfloat16)

def reference(tokens, norm_gain, routing, gate_share, w_gate, w_up, w_down):
    normed = norm_rows(tokens, norm_gain)
    experts = w_gate.shape[0]
    room_size = N_EP * CAP
    onehot = (routing[:, :, None] == jnp.arange(experts, dtype=jnp.int32)[None, None, :]).astype(jnp.int32)
    naming = lax.optimization_barrier(jnp.sum(onehot, axis=1)).astype(jnp.int32)
    ranking = (jnp.cumsum(naming, axis=0) - 1).astype(jnp.int32)

    def run_expert(expert):
        row_ids = jnp.nonzero(naming[:, expert] > 0, size=room_size, fill_value=0)[0].astype(jnp.int32)
        picked = normed[row_ids]
        gate_sum = jnp.dot(picked, w_gate[expert], preferred_element_type=jnp.float32)
        up_sum = jnp.dot(picked, w_up[expert], preferred_element_type=jnp.float32)
        hidden = (jax.nn.silu(gate_sum) * up_sum).astype(jnp.bfloat16)
        return jnp.dot(hidden, w_down[expert], preferred_element_type=jnp.float32).astype(jnp.bfloat16)
    outputs = lax.map(run_expert, jnp.arange(experts, dtype=jnp.int32))
    position = jnp.take_along_axis(ranking, routing, axis=1).astype(jnp.int32)
    picked_out = outputs[routing, position]
    mixed_out = lax.optimization_barrier(jnp.sum(gate_share[:, :, None] * picked_out.astype(jnp.float32), axis=1))
    return mixed_out.astype(jnp.bfloat16)
```

```python
import jax
import jax.numpy as jnp
from jax import lax
from jax.experimental import pallas as pl
from jax.experimental.pallas import tpu as pltpu
from jax.sharding import Mesh, PartitionSpec as P

epsilon = 1e-06
LANES = 128
F32 = jnp.float32
BF16 = jnp.bfloat16


def token_columns(first, rows, routing_ref, share_ref):
    count = routing_ref.shape[1]
    lane = lax.broadcasted_iota(jnp.int32, (rows, count), 1)
    row = lax.broadcasted_iota(jnp.int32, (rows, count), 0)
    hit = lane == row + first
    ids = [
        jnp.sum(jnp.where(hit, routing_ref[k : k + 1, :], 0), axis=1, keepdims=True) for k in (0, 1)
    ]
    shares = [
        jnp.sum(jnp.where(hit, share_ref[k : k + 1, :], 0.0), axis=1, keepdims=True) for k in (0, 1)
    ]
    return ids, shares


def pack_kernel(tp_ref, tokens_ref, gain_ref, routing_ref, share_ref, out_ref):
    copies, rows, _ = out_ref.shape
    width = tokens_ref.shape[1]
    as_float = tokens_ref[...].astype(F32)
    mean = jnp.mean(as_float * as_float, axis=-1, keepdims=True)
    normed = (as_float * lax.rsqrt(mean + epsilon) * gain_ref[...]).astype(BF16)
    ids, shares = token_columns(tp_ref[0] * rows, rows, routing_ref, share_ref)
    columns = [ids[0].astype(F32), ids[1].astype(F32)]
    for share in shares:
        high = share.astype(BF16).astype(F32)
        middle = (share - high).astype(BF16).astype(F32)
        low = share - high - middle
        columns += [high, middle, low]
    lane = lax.broadcasted_iota(jnp.int32, (rows, LANES), 1)
    extra = jnp.zeros((rows, LANES), F32)
    for at, column in enumerate(columns):
        extra = jnp.where(lane == at, column, extra)
    extra = extra.astype(BF16)
    for copy in range(copies):
        out_ref[copy, :, :width] = normed
        out_ref[copy, :, width:] = extra


def expert_kernel(ep_ref, rows_ref, own_ref, other_ref, out_ref):
    groups, rows, packed = rows_ref.shape
    width = packed - LANES
    local = own_ref.shape[2]
    everything = rows_ref[...].reshape(groups * rows, packed)
    x = everything[:, :width]
    extra = everything[:, width:].astype(F32)

    def weight(kind, expert):
        halves = [r[:, kind, expert].reshape(-1, width) for r in (own_ref, other_ref)]
        return jnp.concatenate(halves, axis=0)

    outs = []
    for expert in range(local):
        nt = (((1,), (1,)), ((), ()))
        gate = lax.dot_general(x, weight(0, expert), nt, preferred_element_type=F32)
        up = lax.dot_general(x, weight(1, expert), nt, preferred_element_type=F32)
        hidden = (gate / (1.0 + jnp.exp(-gate)) * up).astype(BF16)
        outs.append(jnp.dot(hidden, weight(2, expert), preferred_element_type=F32).astype(BF16))
    first = ep_ref[0] * local
    id0 = extra[:, 0:1].astype(jnp.int32) - first
    id1 = extra[:, 1:2].astype(jnp.int32) - first
    share0 = (extra[:, 2:3] + extra[:, 3:4]) + extra[:, 4:5]
    share1 = (extra[:, 5:6] + extra[:, 6:7]) + extra[:, 7:8]
    here0 = (id0 == 0) | (id0 == 1)
    here1 = (id1 == 0) | (id1 == 1)
    both = here0 & here1
    zero, one = outs[0].astype(F32), outs[1].astype(F32)
    pick0 = jnp.where(id0 == 0, zero, one)
    pick1 = jnp.where(id1 == 0, zero, one)
    mixed = share0 * pick0 + share1 * pick1
    result = jnp.where(both, mixed, jnp.where(here0, pick0, pick1))
    out_ref[...] = result.astype(BF16).reshape(groups, rows, width)


def combine_kernel(tp_ref, back_ref, routing_ref, share_ref, out_ref):
    sources, rows, width = back_ref.shape
    parts, _, columns = out_ref.shape
    ids, shares = token_columns(tp_ref[0] * rows, rows, routing_ref, share_ref)
    owner0, owner1 = ids[0] // 2, ids[1] // 2
    pick0 = jnp.zeros((rows, width), F32)
    pick1 = jnp.zeros((rows, width), F32)
    for source in range(sources):
        block = back_ref[source].astype(F32)
        pick0 = jnp.where(owner0 == source, block, pick0)
        pick1 = jnp.where(owner1 == source, block, pick1)
    mixed = shares[0] * pick0 + shares[1] * pick1
    result = jnp.where(owner0 == owner1, pick0, mixed).astype(BF16)
    for part in range(parts):
        out_ref[part] = result[:, part * columns : (part + 1) * columns]


def whole(*shape):
    return pl.BlockSpec(memory_space=pltpu.VMEM)


def body(tokens, norm_gain, routing, gate_share, w_gate, w_up, w_down):
    ep = ("y", "x")
    tp = ("z", "c")
    ep_size, tp_size = lax.axis_size(ep), lax.axis_size(tp)
    rows, width = tokens.shape
    ep_index = lax.axis_index(ep).astype(jnp.int32).reshape(1)
    tp_index = lax.axis_index(tp).astype(jnp.int32).reshape(1)
    routing_t, share_t = routing.T, gate_share.T
    smem = pl.BlockSpec(memory_space=pltpu.SMEM)
    vmem = pl.BlockSpec(memory_space=pltpu.VMEM)

    shards = jnp.stack([w_gate.transpose(0, 2, 1), w_up.transpose(0, 2, 1), w_down])
    own = lax.all_gather(shards, "z")

    packed = pl.pallas_call(
        pack_kernel,
        out_shape=jax.ShapeDtypeStruct((ep_size, rows, width + LANES), BF16),
        in_specs=[smem, vmem, vmem, vmem, vmem],
        out_specs=vmem,
        name="pack",
    )(tp_index, tokens, norm_gain.reshape(1, width), routing_t, share_t)
    landed = lax.all_to_all(packed, ep, 0, 0, tiled=True)
    own, landed = lax.optimization_barrier((own, landed))
    other = lax.ppermute(own, "c", [(0, 1), (1, 0)])
    produced = pl.pallas_call(
        expert_kernel,
        out_shape=jax.ShapeDtypeStruct((ep_size, rows, width), BF16),
        in_specs=[smem, vmem, vmem, vmem],
        out_specs=vmem,
        name="experts",
    )(ep_index, landed, own, other)
    back = lax.all_to_all(produced, ep, 0, 0, tiled=True)
    leaving = pl.pallas_call(
        combine_kernel,
        out_shape=jax.ShapeDtypeStruct((tp_size, rows, width // tp_size), BF16),
        in_specs=[smem, vmem, vmem, vmem],
        out_specs=vmem,
        name="combine",
    )(tp_index, back, routing_t, share_t)
    arrived = lax.all_to_all(leaving, tp, 0, 0, tiled=True)
    return arrived.reshape(tp_size * rows, width // tp_size)


def solution(mesh):
    ep, tp = ("y", "x"), ("z", "c")
    fine = Mesh(mesh.devices.reshape(4, 4, 8, 2), ep + tp)
    return jax.shard_map(
        body,
        mesh=fine,
        in_specs=(
            P(ep + tp, None),
            P(),
            P(ep, None),
            P(ep, None),
            P(ep, None, tp),
            P(ep, None, tp),
            P(ep, tp, None),
        ),
        out_specs=P(ep, tp),
        check_vma=False,
    )
```
